32 devices in a mesh: sp: 16 (over z, y, x), tp: 2 (over core).
Axes of the slice: x: 2, y: 2, z: 4, core: 2. Of those that a mesh axis runs over, the one named last changes fastest.
Arguments:
- cotangent: bfloat16 [3072, 2048], P('sp'), may hold values from -0.59765625 to 0.59765625
- mixed_input: bfloat16 [3072, 2048], P('sp'), may hold values from -6 to 6
- route_ids: int32 [3072, 2], P('sp'), may hold values from 0 to 15, all different within a row; in each aligned block of 192 rows (0 to 191, 192 to 383, ...) at most 48 rows name the same one
- route_gates: float32 [3072, 2], P('sp'), may hold values from 0.25 to 1.5
- expert_gate: bfloat16 [16, 2048, 1024], P('sp', None, 'tp'), may hold values from -0.125 to 0.125
- expert_up: bfloat16 [16, 2048, 1024], P('sp', None, 'tp'), may hold values from -0.125 to 0.125
- expert_down: bfloat16 [16, 1024, 2048], P('sp', 'tp'), may hold values from -0.1875 to 0.1875
- projection: bfloat16 [2048, 1024], P(None, 'tp'), may hold values from -0.1875 to 0.1875
- mixer_output: bfloat16 [3072, 1024], P('sp', 'tp'), may hold values from -6 to 6
- query_rows: bfloat16 [3072, 512], P('sp', 'tp'), may hold values from -6 to 6
- key_rows: bfloat16 [3072, 512], P('sp', 'tp'), may hold values from -0.75 to 0.75
- value_rows: bfloat16 [3072, 1024], P('sp', 'tp'), may hold values from -6 to 6
- log_forward: float32 [3072, 512], P('sp', 'tp'), may hold values from -0.25 to 0, as said below
- log_backward: float32 [3072, 512], P('sp', 'tp'), may hold values from -0.25 to 0, as said below
Outputs:
- gate_grad: float32 [16, 2048, 1024], P('sp', None, 'tp')
- up_grad: float32 [16, 2048, 1024], P('sp', None, 'tp')
- down_grad: float32 [16, 1024, 2048], P('sp', 'tp')
- projection_grad: float32 [2048, 1024], P('sp', 'tp')
- query_grad: float32 [3072, 512], P('sp', 'tp')
- key_grad: float32 [3072, 512], P('sp', 'tp')
- value_grad: float32 [3072, 1024], P('sp', 'tp')
- log_forward_grad: float32 [3072, 512], P('sp', 'tp')
- log_backward_grad: float32 [3072, 512], P('sp', 'tp')
The draws below stay inside these ranges and needn't reach their ends.
Inputs may be any that keep to these rules, and one draw needn't show every extreme that they name: `route_ids`: in the rows of one device no expert is named by more than 48 routes, a bound that some block reaches in the rows of some device; the 2 experts of a token differ. `log_forward`: strictly negative. `log_backward`: strictly negative.
All inputs are finite; a program needn't handle non-finite values.
Results may differ from the reference program's by a relative error of at most 0.006.
Values may be sent and summed in bfloat16 or wider, within the bound.
A program may use at most 192 MiB of HBM per device.

```python
import math
import jax
import jax.numpy as jnp
import numpy as np
from jax import lax

D = 2048
F = 1024
HEADS = 16
DK = 32
DV = 64
BLK = 64
TOP = 2
TOK_DEV = 192
TOKENS = 3072
EXPERTS = 16
CAP = 48
QW = 512
VW = 1024
N_SP = 16
N_TP = 2


def decay_table(base_key):
    subkeys = jax.random.split(base_key, 6)
    slow_share = 0.5
    slow_mask = jax.random.uniform(subkeys[0], (QW,), jnp.float32) < slow_share
    slow_rate = jnp.exp(jax.random.uniform(subkeys[1], (QW,), jnp.float32, math.log(0.3), math.log(1.5))) / TOKENS
    fast_rate = jnp.exp(jax.random.uniform(subkeys[2], (QW,), jnp.float32, math.log(0.01), math.log(1.0 / 30.0)))
    rates = jnp.where(slow_mask, slow_rate, fast_rate)
    block_factor = jnp.repeat(jnp.exp(jax.random.uniform(subkeys[3], (TOKENS // BLK, QW), jnp.float32, -0.7, 0.7)), BLK, axis=0)
    device_factor = jnp.repeat(jnp.exp(jax.random.uniform(subkeys[4], (TOKENS // TOK_DEV, QW), jnp.float32, -0.7, 0.7)), TOK_DEV, axis=0)
    roughness = jax.random.uniform(subkeys[5], (TOKENS, QW), jnp.float32, 0.5, 1.5)
    return -(rates[None, :] * block_factor * device_factor * roughness)


def draw_log_forward(key, part):
    return decay_table(jax.random.fold_in(key, 11))


def draw_log_backward(key, part):
    return decay_table(jax.random.fold_in(key, 12))


def raised(entries, key, source, target, shards_of, factor):
    owner, partner = [(jnp.arange(entries.shape[axis_at]) // (entries.shape[axis_at] // shards_of)).reshape([-1 if axis == axis_at else 1 for axis in range(entries.ndim)]) for axis_at in (source, target)]
    chosen = jax.random.permutation(key, shards_of)[partner]
    strong = (owner == chosen) | (owner == (partner + shards_of // 2) % shards_of)
    return jnp.where(strong, factor * entries, entries)


def block_levels(own_key, dims, pieces, low, largest):
    loudness = 1.0
    for dim, blocks in pieces:
        draws = jax.random.uniform(jax.random.fold_in(jax.random.fold_in(own_key, 6), dim), (blocks,), jnp.float32, low / len(pieces), largest / len(pieces))
        loudness = loudness * jnp.repeat(jnp.exp(draws), dims[dim] // blocks).reshape((-1,) + (1,) * (len(dims) - 1 - dim))
    return loudness


def deal_out(own_key, own, number, rows, count, top, reach, lean):
    ranking = jax.random.permutation(own_key, count)
    heavy_load, usual = load_shares(count, rows * top, reach, lean, True), load_shares(count, rows * top, reach, lean, False)
    places = jnp.arange(count)

    def named(lengths, offset_by):
        used = int((lengths > 0).sum())
        fixed = max(1, used // 4)
        shifted = fixed + (places - fixed + offset_by * (used - fixed)) % max(1, count - fixed)
        return jnp.zeros((count,), jnp.int32).at[ranking[jnp.where(places < fixed, places, shifted)]].set(jnp.asarray(lengths, jnp.int32))

    lengths = jnp.where(number % 4 == 0, named(heavy_load, number // 4), named(usual, number - number // 4 - 1))
    mixed = jax.random.permutation(jax.random.fold_in(own, 3), count)
    giver, receiver = mixed[0:count // 2 * 2:2], mixed[1:count // 2 * 2:2]
    margin = jnp.minimum(lengths[giver] - 1, reach - lengths[receiver]) // 2
    margin = jnp.where((giver == ranking[0]) | (receiver == ranking[0]) | (lengths[receiver] == 0), 0, jnp.maximum(margin, 0))
    shifted = jax.random.randint(jax.random.fold_in(own, 4), (count // 2,), 0, 1 << 20) % (margin + 1)
    lengths = lengths.at[giver].add(-shifted).at[receiver].add(shifted)
    labels = jnp.searchsorted(jnp.cumsum(lengths), jnp.arange(rows * top), side="right").astype(jnp.int32)
    table = labels.reshape(top, rows).T
    table = table[jax.random.permutation(jax.random.fold_in(own, 1), rows)]
    offset_by = jax.random.randint(jax.random.fold_in(own, 2), (rows, 1), 0, top)
    return jnp.take_along_axis(table, (jnp.arange(top)[None, :] + offset_by) % top, axis=1)


def load_shares(amount, total, bound, skew, full):
    loads = [(1 << 20) // math.isqrt(standing ** skew) + 1 for standing in range(1, amount + 1)]
    largest = bound if full else min(bound, max(-(-total // amount), total * loads[0] // sum(loads)))
    least = 1 if total - largest >= amount - 1 else 0
    counts, spare = [largest] + [least] * (amount - 1), total - largest - least * (amount - 1)
    while spare > 0:
        candidates = [i for i in range(1, amount) if counts[i] < largest] or [i for i in range(1, amount) if counts[i] < bound]
        mass, remaining = sum([loads[i] for i in candidates]), spare
        for i in candidates:
            addition = min(bound - counts[i], max(1, remaining * loads[i] // mass), spare)
            counts[i] = counts[i] + addition
            spare = spare - addition
    return np.array(counts)


def normal_values(key, shape, scale, limit, cuts=(), held_as=jnp.bfloat16):
    values = scale * jax.random.normal(key, shape, jnp.float32)
    if cuts:
        values = values * block_levels(key, shape, cuts, -0.22, 0.18)
    return jnp.clip(values, -limit, limit).astype(held_as)


def heavy_noise(own_key, shape, width, most, shards, heavy, kind=jnp.bfloat16):
    values = width * jax.random.normal(own_key, shape, jnp.float32)
    if shards:
        values = values * block_levels(own_key, shape, shards, -0.22, 0.18)
    return jnp.clip(raised(values, jax.random.fold_in(own_key, 3), *heavy), -most, most).astype(kind)


def setup_inputs(seed: int = 0) -> dict:
    arg_keys = jax.random.split(jax.random.key(seed), 15)
    cotangent = heavy_noise(arg_keys[0], (TOKENS, D), 0.1, 0.59765625, ((0, 16),), (0, 1, 16, 2.0))
    mixed_input = normal_values(arg_keys[1], (TOKENS, D), 1.0, 6.0, ((0, 16),))
    route_ids_keys = jax.random.split(jax.random.fold_in(arg_keys[2], 1), TOKENS // TOK_DEV)
    route_ids_turns = jax.random.permutation(jax.random.fold_in(arg_keys[2], 3), TOKENS // TOK_DEV)
    route_ids = jax.vmap(lambda own, number: deal_out(jax.random.fold_in(arg_keys[2], 2), own, number, TOK_DEV, EXPERTS, TOP, CAP, 2))(route_ids_keys, route_ids_turns).reshape((TOKENS, TOP))
    route_gates = jnp.clip(0.25 + 1.25 * jax.random.uniform(arg_keys[3], (TOKENS, TOP), jnp.float32) ** block_levels(arg_keys[3], (TOKENS, TOP), ((0, 16),), -0.2, 0.2), 0.25, 1.5)
    expert_gate = normal_values(arg_keys[4], (EXPERTS, D, F), D ** -0.5, 0.125, ((0, 16), (2, 2)))
    expert_up = normal_values(arg_keys[5], (EXPERTS, D, F), D ** -0.5, 0.125, ((0, 16), (2, 2)))
    expert_down = normal_values(arg_keys[6], (EXPERTS, F, D), F ** -0.5, 0.1875, ((0, 16), (1, 2)))
    projection = normal_values(arg_keys[7], (D, VW), VW ** -0.5, 0.1875, ((1, 2),))
    mixer_output = normal_values(arg_keys[8], (TOKENS, VW), 1.0, 6.0, ((0, 16), (1, 2)))
    query_rows = normal_values(arg_keys[9], (TOKENS, QW), 1.0, 6.0, ((0, 16), (1, 2)))
    key_rows = normal_values(arg_keys[10], (TOKENS, QW), 0.125, 0.75, ((0, 16), (1, 2)))
    value_rows = normal_values(arg_keys[11], (TOKENS, VW), 1.0, 6.0, ((0, 16), (1, 2)))
    log_forward = draw_log_forward(jax.random.fold_in(arg_keys[14], 71), 0)
    log_backward = draw_log_backward(jax.random.fold_in(arg_keys[14], 71), 0)
    return {"cotangent": cotangent, "mixed_input": mixed_input, "route_ids": route_ids, "route_gates": route_gates, "expert_gate": expert_gate, "expert_up": expert_up, "expert_down": expert_down, "projection": projection, "mixer_output": mixer_output, "query_rows": query_rows, "key_rows": key_rows, "value_rows": value_rows, "log_forward": log_forward, "log_backward": log_backward}


topmost_precision = lax.Precision.HIGHEST

def decayed_pass(query_stack, key_matrix, value_matrix, log_rate, entering):
    count = query_stack.shape[0]
    head_count = query_stack.shape[1]
    key_width = query_stack.shape[2]
    value_width = value_matrix.shape[2]
    blocks = count // BLK
    query_blocks = query_stack.reshape(blocks, BLK, head_count, key_width)
    key_blocks = key_matrix.reshape(blocks, BLK, head_count, key_width)
    value_blocks = value_matrix.reshape(blocks, BLK, head_count, value_width)
    running_prefix = jnp.cumsum(log_rate.reshape(blocks, BLK, head_count, key_width), axis=1)
    last_cum = running_prefix[:, -1:]
    increment = jnp.einsum('nlhk,nlhv->nhkv', key_blocks * jnp.exp(last_cum - running_prefix), value_blocks, precision=topmost_precision)
    decay = jnp.exp(last_cum[:, 0])

    def advance(carried, inputs):
        factor, added = inputs
        return (factor[..., None] * carried + added, carried)
    final_state, entering_states = lax.scan(advance, entering, (decay, increment))
    inter_part = jnp.einsum('nlhk,nhkv->nlhv', query_blocks * jnp.exp(running_prefix), entering_states, precision=topmost_precision)
    middle = running_prefix[:, BLK // 2 - 1:BLK // 2]
    scores = jnp.einsum('nlhk,nmhk->nhlm', query_blocks * jnp.exp(running_prefix - middle), key_blocks * jnp.exp(middle - running_prefix), precision=topmost_precision)
    lower_mask = jnp.tril(jnp.ones((BLK, BLK), bool))
    scores = jnp.where(lower_mask, scores, jnp.float32(0.0))
    intra_part = jnp.einsum('nhlm,nmhv->nlhv', scores, value_blocks, precision=topmost_precision)
    return ((inter_part + intra_part).reshape(count, head_count, value_width), final_state)

def reverse_rows(source_array):
    return jnp.flip(source_array, axis=0)

def whole_mixer(query_in, key_in, value_in, forward_in, backward_in):
    query_scaling = DK ** (-0.5)
    entering = jnp.zeros((HEADS, DK, DV), jnp.float32)
    out_fwd, _ = decayed_pass(query_in * query_scaling, key_in, value_in, forward_in, entering)
    out_bwd, _ = decayed_pass(reverse_rows(query_in) * query_scaling, reverse_rows(key_in), reverse_rows(value_in), reverse_rows(backward_in), entering)
    return out_fwd + reverse_rows(out_bwd)

def reference(cotangent, mixed_input, route_ids, route_gates, expert_gate, expert_up, expert_down, projection, mixer_output, query_rows, key_rows, value_rows, log_forward, log_backward):
    flat_ids = route_ids.reshape(-1)
    route_total = TOKENS * TOP
    row_limit = N_SP * CAP
    unit_share = F // N_TP
    gate_padded = jnp.concatenate([route_gates.reshape(-1), jnp.zeros((1,), jnp.float32)])
    cot_padded = jnp.concatenate([cotangent, jnp.zeros((1, D), jnp.bfloat16)], axis=0)
    input_padded = jnp.concatenate([mixed_input, jnp.zeros((1, D), jnp.bfloat16)], axis=0)

    def per_expert(gathered_sum, expert_index):
        found = jnp.nonzero(flat_ids == expert_index, size=row_limit, fill_value=route_total)[0].astype(jnp.int32)
        token_of = (found // TOP).astype(jnp.int32)
        routed = (gate_padded[found][:, None] * cot_padded[token_of].astype(jnp.float32)).astype(jnp.bfloat16)
        tok_rows = input_padded[token_of]
        w_gate = expert_gate[expert_index]
        w_up = expert_up[expert_index]
        w_down = expert_down[expert_index]
        gate_pre = jnp.dot(tok_rows, w_gate, preferred_element_type=jnp.float32)
        up_pre = jnp.dot(tok_rows, w_up, preferred_element_type=jnp.float32)
        sigmoid_gate = jax.nn.sigmoid(gate_pre)
        silu_gate = gate_pre * sigmoid_gate
        hidden = (silu_gate * up_pre).astype(jnp.bfloat16)
        hidden_grad = jnp.dot(routed, w_down.T, preferred_element_type=jnp.float32)
        slope = sigmoid_gate * (1.0 + gate_pre * (1.0 - sigmoid_gate))
        gate_pre_grad = (hidden_grad * up_pre * slope).astype(jnp.bfloat16)
        up_pre_grad = (hidden_grad * silu_gate).astype(jnp.bfloat16)
        down_term = jnp.dot(hidden.T, routed, preferred_element_type=jnp.float32)
        gate_term = jnp.dot(tok_rows.T, gate_pre_grad, preferred_element_type=jnp.float32)
        up_term = jnp.dot(tok_rows.T, up_pre_grad, preferred_element_type=jnp.float32)
        row_grad = jnp.zeros((row_limit, D), jnp.float32)
        for portion in range(N_TP):
            start_unit = portion * unit_share
            end_unit = start_unit + unit_share
            partial_value = jnp.dot(gate_pre_grad[:, start_unit:end_unit], w_gate[:, start_unit:end_unit].T, preferred_element_type=jnp.float32)
            partial_value = partial_value + jnp.dot(up_pre_grad[:, start_unit:end_unit], w_up[:, start_unit:end_unit].T, preferred_element_type=jnp.float32)
            rounded = lax.optimization_barrier(partial_value.astype(jnp.bfloat16))
            row_grad = row_grad + rounded.astype(jnp.float32)
        row_grad = row_grad.astype(jnp.bfloat16)
        gathered_sum = gathered_sum.at[token_of].add(row_grad.astype(jnp.float32))
        return (gathered_sum, (gate_term, up_term, down_term))
    gathered, expert_terms = lax.scan(per_expert, jnp.zeros((TOKENS + 1, D), jnp.float32), jnp.arange(EXPERTS, dtype=jnp.int32))
    mid_grad = (gathered[:TOKENS] + cotangent.astype(jnp.float32)).astype(jnp.bfloat16)
    mix_grad = jnp.dot(mid_grad, projection, preferred_element_type=jnp.float32).astype(jnp.bfloat16)
    projection_grad = jnp.dot(mid_grad.T, mixer_output, preferred_element_type=jnp.float32)

    def by_heads(source_array, head_width):
        return source_array.astype(jnp.float32).reshape(TOKENS, HEADS, head_width)
    _, pullback = jax.vjp(whole_mixer, by_heads(query_rows, DK), by_heads(key_rows, DK), by_heads(value_rows, DV), by_heads(log_forward, DK), by_heads(log_backward, DK))
    grads = pullback(by_heads(mix_grad, DV))
    query_grad = grads[0].reshape(TOKENS, QW)
    key_grad = grads[1].reshape(TOKENS, QW)
    value_grad = grads[2].reshape(TOKENS, VW)
    log_forward_grad = grads[3].reshape(TOKENS, QW)
    log_backward_grad = grads[4].reshape(TOKENS, QW)
    return (expert_terms[0], expert_terms[1], expert_terms[2], projection_grad, query_grad, key_grad, value_grad, log_forward_grad, log_backward_grad)
```

```python
import functools

import jax
import jax.numpy as jnp
from jax import lax
from jax.experimental import pallas as pl
from jax.experimental.pallas import tpu as pltpu
from jax.sharding import PartitionSpec as P

DK = 32
DV = 64
F32 = jnp.float32
BF16 = jnp.bfloat16
MESH = pl.DeviceIdType.MESH
HIGHEST = lax.Precision.HIGHEST
VMEM = pl.BlockSpec(memory_space=pltpu.VMEM)
ANY = pl.BlockSpec(memory_space=pl.ANY)
VMEM_LIMIT = 60 * 1024 * 1024


def dot(a, b, dims=((1,), (0,)), precision=None):
    return lax.dot_general(a, b, (dims, ((), ())), preferred_element_type=F32, precision=precision)


def triangle(count, lower):
    rows = lax.broadcasted_iota(jnp.int32, (count, count), 0)
    cols = lax.broadcasted_iota(jnp.int32, (count, count), 1)
    return rows >= cols if lower else rows <= cols


def head_lanes(head, width, total):
    lane = lax.broadcasted_iota(jnp.int32, (1, total), 1)
    return (lane >= head * width) & (lane < (head + 1) * width)


def block_states(wide, narrow, heads):
    full = dot(wide, narrow, ((0,), (0,)))
    keys = narrow.shape[1]
    total = jnp.zeros((DV, keys), F32)
    for head in range(heads):
        total = jnp.where(head_lanes(head, DK, keys), full[head * DV : (head + 1) * DV], total)
    return total


def prep_kernel(heads, k_ref, v_ref, lf_ref, lb_ref, cf_ref, cb_ref, tot_ref, st_ref, sb_ref):
    count, keys = k_ref.shape
    lower = triangle(count, True).astype(F32)
    upper = triangle(count, False).astype(F32)
    cf = dot(lower, lf_ref[...], precision=HIGHEST)
    cb = dot(upper, lb_ref[...], precision=HIGHEST)
    cf_ref[...] = cf
    cb_ref[...] = cb
    tf = cf[count - 1 : count]
    tb = cb[0:1]
    tot_ref[:, :keys] = jnp.broadcast_to(tf, (8, keys))
    tot_ref[:, keys:] = jnp.broadcast_to(tb, (8, keys))
    k = k_ref[...].astype(F32)
    v = v_ref[...]
    for slot, (total, running) in enumerate(((tf, cf), (tb, cb))):
        state = block_states(v, (k * jnp.exp(total - running)).astype(BF16), heads)
        st_ref[slot] = state
        sb_ref[slot] = state.astype(BF16)


def pull_kernel(heads, q_ref, do_ref, cf_ref, cb_ref, pulled_ref):
    q = q_ref[...].astype(F32) * (DK**-0.5)
    do = do_ref[...]
    for slot, ref in ((0, cb_ref), (1, cf_ref)):
        pulled_ref[slot] = block_states(do, (q * jnp.exp(ref[...])).astype(BF16), heads).astype(BF16)


def send_all(count, me, make):
    barrier = pltpu.get_barrier_semaphore()
    for step in range(1, count):
        pl.semaphore_signal(
            barrier, inc=1, device_id={"sp": lax.rem(me + step, count)}, device_id_type=MESH
        )
    pl.semaphore_wait(barrier, count - 1)
    copies = []
    for step in range(1, count):
        for copy in make(step, lax.rem(me + step, count), (me + step) // count):
            copy.start()
            copies.append(copy)
    for copy in copies:
        copy.wait()


def chain(count, me, slots, totals, low_cols, high_cols, out_ref):
    shape = out_ref.shape[1:]
    low = jnp.zeros(shape, F32)
    high = jnp.zeros(shape, F32)
    for step in range(count - 1, 0, -1):
        use = (me >= step).astype(F32)
        decay = jnp.exp(totals[step, 0:1, low_cols])
        low = (1.0 - use + use * decay) * low + use * slots[step].astype(F32)
    for step in range(1, count):
        use = (me < step).astype(F32)
        decay = jnp.exp(totals[step, 0:1, high_cols])
        high = (1.0 - use + use * decay) * high + use * slots[step].astype(F32)
    out_ref[0] = low
    out_ref[1] = high


def first_exchange(count, x_ref, tot_ref, out_ref, totals_ref, slots, got, send, recv, tsend, trecv):
    me = lax.axis_index("sp")
    keys = x_ref.shape[2]

    def make(step, target, half):
        return (
            pltpu.make_async_remote_copy(
                src_ref=x_ref.at[half], dst_ref=slots.at[step], send_sem=send.at[step],
                recv_sem=recv.at[step], device_id={"sp": target}, device_id_type=MESH,
            ),
            pltpu.make_async_remote_copy(
                src_ref=tot_ref, dst_ref=got.at[step], send_sem=tsend.at[step],
                recv_sem=trecv.at[step], device_id={"sp": target}, device_id_type=MESH,
            ),
        )

    send_all(count, me, make)
    totals_ref[0] = tot_ref[...]
    for step in range(1, count):
        totals_ref[step] = got[step]
    chain(count, me, slots, got, slice(0, keys), slice(keys, 2 * keys), out_ref)


def second_exchange(count, x_ref, totals_ref, out_ref, slots, send, recv):
    me = lax.axis_index("sp")
    keys = x_ref.shape[2]

    def make(step, target, half):
        return (
            pltpu.make_async_remote_copy(
                src_ref=x_ref.at[half], dst_ref=slots.at[step], send_sem=send.at[step],
                recv_sem=recv.at[step], device_id={"sp": target}, device_id_type=MESH,
            ),
        )

    send_all(count, me, make)
    chain(count, me, slots, totals_ref, slice(keys, 2 * keys), slice(0, keys), out_ref)


def grads_kernel(
    heads, q_ref, k_ref, v_ref, do_ref, cf_ref, cb_ref, st_ref, into_ref, leave_ref,
    dq_ref, dk_ref, dv_ref, df_ref, db_ref,
):
    count, keys = k_ref.shape
    scale = DK**-0.5
    q = q_ref[...].astype(F32) * scale
    k = k_ref[...].astype(F32)
    v = v_ref[...]
    do = do_ref[...]
    lower = triangle(count, True)
    upper = triangle(count, False)
    sides = []
    dv = None
    for side in range(2):
        running = (cf_ref, cb_ref)[side][...]
        total = running[count - 1 : count] if side == 0 else running[0:1]
        up = jnp.exp(running - 0.5 * total)
        down = jnp.exp(0.5 * total - running)
        entering = into_ref[side]
        leaving = leave_ref[1 - side]
        spread_in = jnp.concatenate(
            [jnp.where(head_lanes(h, DK, keys), entering, 0.0) for h in range(heads)], axis=0
        ).astype(BF16)
        spread_out = jnp.concatenate(
            [jnp.where(head_lanes(h, DK, keys), leaving, 0.0) for h in range(heads)], axis=0
        ).astype(BF16)
        tail = jnp.exp(total - running)
        dq = jnp.exp(running) * dot(do, spread_in)
        dk = tail * dot(v, spread_out)
        part = dot((k * tail).astype(BF16), spread_out, ((1,), (1,)))
        dv = part if dv is None else dv + part
        edge = jnp.sum((jnp.exp(total) * entering + st_ref[side]) * leaving, axis=0, keepdims=True)
        sides.append([(q * up).astype(BF16), (k * down).astype(BF16), up, down, dq, dk, edge])
    dv_ref[...] = dv
    inner = [[jnp.zeros((count, keys), F32) for _ in range(2)] for _ in range(2)]
    for head in range(heads):
        pair = slice(head // 2 * 2 * DV, (head // 2 * 2 + 2) * DV)
        half = head_lanes(head % 2, DV, 2 * DV)
        mask = head_lanes(head, DK, keys)
        do_pair = jnp.where(half, do[:, pair], jnp.zeros((), BF16))
        v_pair = v[:, pair]
        weights = dot(do_pair, v_pair, ((1,), (1,)))
        turned = dot(v_pair, do_pair, ((1,), (1,)))
        mixed = None
        for side in range(2):
            q_side, k_side = sides[side][:2]
            q_head = jnp.where(mask, q_side, jnp.zeros((), BF16))
            k_head = jnp.where(mask, k_side, jnp.zeros((), BF16))
            kept, kept_turned = (lower, upper) if side == 0 else (upper, lower)
            scores = jnp.where(kept_turned, dot(k_head, q_side, ((1,), (1,))), 0.0)
            mixed = scores if mixed is None else mixed + scores
            inner[side][0] += dot(jnp.where(kept, weights, 0.0).astype(BF16), k_head)
            inner[side][1] += dot(jnp.where(kept_turned, turned, 0.0).astype(BF16), q_head)
        dv_ref[:, pair] += dot(mixed.astype(BF16), do_pair)
    total_q = None
    for side in range(2):
        up, down, dq, dk, edge = sides[side][2:]
        dq = dq + up * inner[side][0]
        dk = dk + down * inner[side][1]
        gap = q * dq - k * dk
        sums = (upper if side == 0 else lower).astype(F32)
        (df_ref, db_ref)[side][...] = dot(sums, gap, precision=HIGHEST) + edge
        if side == 0:
            total_q, total_k = dq, dk
        else:
            dq_ref[...] = (total_q + dq) * scale
            dk_ref[...] = total_k + dk


def cost(flops, moved):
    return pl.CostEstimate(flops=flops, bytes_accessed=moved, transcendentals=0)


def params(identity=None):
    if identity is None:
        return pltpu.CompilerParams(vmem_limit_bytes=VMEM_LIMIT)
    return pltpu.CompilerParams(
        collective_id=identity, has_side_effects=True, vmem_limit_bytes=VMEM_LIMIT
    )


def shaped(shape, kind=F32):
    return jax.ShapeDtypeStruct(shape, kind)


def mixer_start(key_rows, value_rows, log_forward, log_backward):
    count, keys = key_rows.shape
    heads = keys // DK
    groups = lax.axis_size("sp")
    cf, cb, total, state, state_sent = pl.pallas_call(
        functools.partial(prep_kernel, heads),
        out_shape=(
            shaped((count, keys)), shaped((count, keys)), shaped((8, 2 * keys)),
            shaped((2, DV, keys)), shaped((2, DV, keys), BF16),
        ),
        in_specs=[VMEM] * 4,
        out_specs=(VMEM,) * 5,
        compiler_params=params(),
        cost_estimate=cost(2 * 10**9, 2 * 10**6),
        name="mixer_prep",
    )(key_rows, value_rows, log_forward, log_backward)
    into, totals = pl.pallas_call(
        functools.partial(first_exchange, groups),
        out_shape=(shaped((2, DV, keys)), shaped((groups, 8, 2 * keys))),
        in_specs=[VMEM] * 2,
        out_specs=(VMEM,) * 2,
        scratch_shapes=[
            pltpu.VMEM((groups, DV, keys), BF16), pltpu.VMEM((groups, 8, 2 * keys), F32),
        ] + [pltpu.SemaphoreType.DMA((groups,))] * 4,
        compiler_params=params(1),
        cost_estimate=cost(10**6, 8 * 10**6),
        name="first_exchange",
    )(state_sent, total)
    return cf, cb, state, into, totals


def mixer_grads(query_rows, key_rows, value_rows, mix_grad, started):
    cf, cb, state, into, totals = started
    count, keys = key_rows.shape
    heads = keys // DK
    groups = lax.axis_size("sp")
    pulled = pl.pallas_call(
        functools.partial(pull_kernel, heads),
        out_shape=shaped((2, DV, keys), BF16),
        in_specs=[VMEM] * 4,
        out_specs=VMEM,
        compiler_params=params(),
        cost_estimate=cost(10**9, 10**6),
        name="mixer_pull",
    )(query_rows, mix_grad, cf, cb)
    leave = pl.pallas_call(
        functools.partial(second_exchange, groups),
        out_shape=shaped((2, DV, keys)),
        in_specs=[VMEM] * 2,
        out_specs=VMEM,
        scratch_shapes=[pltpu.VMEM((groups, DV, keys), BF16)]
        + [pltpu.SemaphoreType.DMA((groups,))] * 2,
        compiler_params=params(2),
        cost_estimate=cost(10**6, 8 * 10**6),
        name="second_exchange",
    )(pulled, totals)
    wide = value_rows.shape[1]
    return pl.pallas_call(
        functools.partial(grads_kernel, heads),
        out_shape=tuple(shaped((count, w)) for w in (keys, keys, wide, keys, keys)),
        in_specs=[VMEM] * 9,
        out_specs=(VMEM,) * 5,
        compiler_params=params(),
        cost_estimate=cost(8 * 10**9, 4 * 10**6),
        name="mixer_grads",
    )(query_rows, key_rows, value_rows, mix_grad, cf, cb, state, into, leave)


def dispatch_kernel(
    count, cot_ref, tok_ref, cot_out, tok_out, send, recv, relay_send, relay_recv, own_sem
):
    me = lax.axis_index("sp")
    core = lax.axis_index("tp")
    partner = 1 - core
    width = cot_ref.shape[2]
    columns = pl.ds(pl.multiple_of(core * width, width), width)
    pairs = ((cot_ref, cot_out), (tok_ref, tok_out))
    barrier = pltpu.get_barrier_semaphore()
    for step in range(1, count):
        pl.semaphore_signal(
            barrier, inc=1, device_id={"sp": lax.rem(me + step, count)}, device_id_type=MESH
        )
    pl.semaphore_signal(barrier, inc=1, device_id={"tp": partner}, device_id_type=MESH)
    pl.semaphore_wait(barrier, count)
    sent = []
    for step in range(1, count):
        target = lax.rem(me + step, count)
        for which, (source, result) in enumerate(pairs):
            copy = pltpu.make_async_remote_copy(
                src_ref=source.at[target],
                dst_ref=result.at[me, :, columns],
                send_sem=send.at[which, step],
                recv_sem=recv.at[which, step],
                device_id={"sp": target},
                device_id_type=MESH,
            )
            copy.start()
            sent.append(copy)
    relayed = []
    for which, (source, result) in enumerate(pairs):
        copy = pltpu.make_async_remote_copy(
            src_ref=source.at[me],
            dst_ref=result.at[me, :, columns],
            send_sem=relay_send.at[which, 0],
            recv_sem=relay_recv.at[which, 0],
            device_id={"tp": partner},
            device_id_type=MESH,
        )
        copy.start()
        relayed.append(copy)
    own = [
        pltpu.make_async_copy(source.at[me], result.at[me, :, columns], own_sem.at[which])
        for which, (source, result) in enumerate(pairs)
    ]
    for copy in own:
        copy.start()
    for step in range(1, count):
        origin = lax.rem(me + count - step, count)
        for which, (source, result) in enumerate(pairs):
            landed = result.at[origin, :, columns]
            pltpu.make_async_remote_copy(
                src_ref=source.at[origin],
                dst_ref=landed,
                send_sem=send.at[which, step],
                recv_sem=recv.at[which, step],
                device_id={"sp": origin},
                device_id_type=MESH,
            ).wait_recv()
            copy = pltpu.make_async_remote_copy(
                src_ref=landed,
                dst_ref=landed,
                send_sem=relay_send.at[which, step],
                recv_sem=relay_recv.at[which, step],
                device_id={"tp": partner},
                device_id_type=MESH,
            )
            copy.start()
            relayed.append(copy)
    for copy in sent:
        copy.wait_send()
    for copy in own:
        copy.wait()
    other = pl.ds(pl.multiple_of(partner * width, width), width)
    for copy in relayed:
        copy.wait_send()
    for step in range(count):
        origin = lax.rem(me + count - step, count)
        for which, (source, result) in enumerate(pairs):
            arrived = result.at[origin, :, other]
            pltpu.make_async_remote_copy(
                src_ref=arrived,
                dst_ref=arrived,
                send_sem=relay_send.at[which, step],
                recv_sem=relay_recv.at[which, step],
                device_id={"tp": partner},
                device_id_type=MESH,
            ).wait_recv()


def dispatch(routed_cot, routed_tok):
    groups, slots, width = routed_cot.shape
    whole = shaped((groups, slots, 2 * width), BF16)
    return pl.pallas_call(
        functools.partial(dispatch_kernel, groups),
        out_shape=(whole, whole),
        in_specs=[ANY] * 2,
        out_specs=(ANY,) * 2,
        scratch_shapes=[pltpu.SemaphoreType.DMA((2, groups))] * 4
        + [pltpu.SemaphoreType.DMA((2,))],
        compiler_params=pltpu.CompilerParams(collective_id=3, has_side_effects=True),
        cost_estimate=cost(10**6, 10**8),
        name="dispatch",
    )(routed_cot, routed_tok)


def local(
    cotangent,
    mixed_input,
    route_ids,
    route_gates,
    expert_gate,
    expert_up,
    expert_down,
    projection,
    mixer_output,
    query_rows,
    key_rows,
    value_rows,
    log_forward,
    log_backward,
):
    tok_count = cotangent.shape[0]
    feature_count = cotangent.shape[1]
    groups = lax.axis_size("sp")
    core = lax.axis_index("tp")
    half = feature_count // 2
    slot_count = 4 * tok_count // groups
    row_total = groups * slot_count
    contract_last = ((1,), (1,))
    contract_first = ((0,), (0,))
    swap = [(0, 1), (1, 0)]

    experts = jnp.arange(groups, dtype=jnp.int32)
    chosen = [(route_ids[:, place : place + 1] == experts[None, :]) for place in range(2)]
    named = (chosen[0] | chosen[1]).astype(BF16)
    steps = jnp.arange(tok_count, dtype=jnp.int32)
    before = dot((steps[:, None] > steps[None, :]).astype(BF16), named)
    place_of = before + (experts * slot_count).astype(F32)[None, :]
    rows = jnp.arange(row_total, dtype=jnp.int32)[:, None]
    hits = []
    for place in range(2):
        target = jnp.sum(jnp.where(chosen[place], place_of, 0.0), axis=1).astype(jnp.int32)
        hits.append(rows == target[None, :])
    pick = (hits[0] | hits[1]).astype(BF16)
    slot_gate = jnp.sum(
        jnp.where(hits[0], route_gates[:, 0][None, :], 0.0)
        + jnp.where(hits[1], route_gates[:, 1][None, :], 0.0),
        axis=1,
        keepdims=True,
    )
    own_cot = lax.dynamic_slice_in_dim(cotangent, core * half, half, 1)
    own_tok = lax.dynamic_slice_in_dim(mixed_input, core * half, half, 1)
    routed_cot = (slot_gate * dot(pick, own_cot)).astype(BF16)
    routed_tok = dot(pick, own_tok).astype(BF16)
    cot_in, tok_in = dispatch(
        routed_cot.reshape(groups, slot_count, half), routed_tok.reshape(groups, slot_count, half)
    )
    started = mixer_start(key_rows, value_rows, log_forward, log_backward)
    w_gate = expert_gate[0]
    w_up = expert_up[0]
    w_down = expert_down[0]
    cot_block = cot_in.reshape(row_total, feature_count)
    tok_block = tok_in.reshape(row_total, feature_count)
    gate_pre = dot(tok_block, w_gate)
    up_pre = dot(tok_block, w_up)
    sigmoid_gate = jax.nn.sigmoid(gate_pre)
    silu_gate = gate_pre * sigmoid_gate
    hidden = (silu_gate * up_pre).astype(BF16)
    hidden_grad = dot(cot_block, w_down, contract_last)
    slope = sigmoid_gate * (1.0 + gate_pre * (1.0 - sigmoid_gate))
    gate_pre_grad = (hidden_grad * up_pre * slope).astype(BF16)
    up_pre_grad = (hidden_grad * silu_gate).astype(BF16)
    partial_value = dot(gate_pre_grad, w_gate, contract_last)
    partial_value = (partial_value + dot(up_pre_grad, w_up, contract_last)).astype(BF16)
    mine = lax.dynamic_slice_in_dim(partial_value, core * half, half, 1)
    other = lax.dynamic_slice_in_dim(partial_value, (1 - core) * half, half, 1)
    came = lax.ppermute(other, "tp", swap)
    summed = (mine.astype(F32) + came.astype(F32)).astype(BF16)
    returned = lax.all_to_all(
        summed.reshape(groups, slot_count, half), "sp", split_axis=0, concat_axis=0, tiled=True
    ).reshape(row_total, half)
    down_term = dot(hidden, cot_block, contract_first)
    gate_term = dot(tok_block, gate_pre_grad, contract_first)
    up_term = dot(tok_block, up_pre_grad, contract_first)
    mid_half = (dot(pick, returned, contract_first) + own_cot.astype(F32)).astype(BF16)
    mid_other = lax.ppermute(mid_half, "tp", swap)
    first = core == 0
    mid_grad = jnp.concatenate(
        [jnp.where(first, mid_half, mid_other), jnp.where(first, mid_other, mid_half)], axis=1
    )
    mix_grad = dot(mid_grad, projection).astype(BF16)
    projection_grad = lax.psum_scatter(
        dot(mid_grad, mixer_output, contract_first), "sp", scatter_dimension=0, tiled=True
    )
    grads = mixer_grads(query_rows, key_rows, value_rows, mix_grad, started)
    return (gate_term[None], up_term[None], down_term[None], projection_grad, *grads)


def solution(mesh):
    rows = P("sp", None)
    both = P("sp", "tp")
    split_last = P("sp", None, "tp")
    split_first = P("sp", "tp", None)
    return jax.shard_map(
        local,
        mesh=mesh,
        in_specs=(
            rows, rows, rows, rows, split_last, split_last, split_first, P(None, "tp"),
            both, both, both, both, both, both,
        ),
        out_specs=(split_last, split_last, split_first, both, both, both, both, both, both),
        check_vma=False,
    )
```

```python
import functools

import jax
import jax.numpy as jnp
from jax import lax
from jax.experimental import pallas as pl
from jax.experimental.pallas import tpu as pltpu
from jax.sharding import PartitionSpec as P

DK = 32
DV = 64
F32 = jnp.float32
BF16 = jnp.bfloat16
MESH = pl.DeviceIdType.MESH
HIGHEST = lax.Precision.HIGHEST
VMEM = pl.BlockSpec(memory_space=pltpu.VMEM)
ANY = pl.BlockSpec(memory_space=pl.ANY)
VMEM_LIMIT = 60 * 1024 * 1024


def dot(a, b, dims=((1,), (0,)), precision=None):
    return lax.dot_general(a, b, (dims, ((), ())), preferred_element_type=F32, precision=precision)


def triangle(count, lower):
    rows = lax.broadcasted_iota(jnp.int32, (count, count), 0)
    cols = lax.broadcasted_iota(jnp.int32, (count, count), 1)
    return rows >= cols if lower else rows <= cols


def head_lanes(head, width, total):
    lane = lax.broadcasted_iota(jnp.int32, (1, total), 1)
    return (lane >= head * width) & (lane < (head + 1) * width)


def block_states(wide, narrow, heads):
    full = dot(wide, narrow, ((0,), (0,)))
    keys = narrow.shape[1]
    total = jnp.zeros((DV, keys), F32)
    for head in range(heads):
        total = jnp.where(head_lanes(head, DK, keys), full[head * DV : (head + 1) * DV], total)
    return total


def prep_kernel(heads, k_ref, v_ref, lf_ref, lb_ref, cf_ref, cb_ref, tot_ref, st_ref, sb_ref):
    count, keys = k_ref.shape
    lower = triangle(count, True).astype(F32)
    upper = triangle(count, False).astype(F32)
    cf = dot(lower, lf_ref[...], precision=HIGHEST)
    cb = dot(upper, lb_ref[...], precision=HIGHEST)
    cf_ref[...] = cf
    cb_ref[...] = cb
    tf = cf[count - 1 : count]
    tb = cb[0:1]
    tot_ref[:, :keys] = jnp.broadcast_to(tf, (8, keys))
    tot_ref[:, keys:] = jnp.broadcast_to(tb, (8, keys))
    k = k_ref[...].astype(F32)
    v = v_ref[...]
    for slot, (total, running) in enumerate(((tf, cf), (tb, cb))):
        state = block_states(v, (k * jnp.exp(total - running)).astype(BF16), heads)
        st_ref[slot] = state
        sb_ref[slot] = state.astype(BF16)


def pull_kernel(heads, q_ref, do_ref, cf_ref, cb_ref, pulled_ref):
    q = q_ref[...].astype(F32) * (DK**-0.5)
    do = do_ref[...]
    for slot, ref in ((0, cb_ref), (1, cf_ref)):
        pulled_ref[slot] = block_states(do, (q * jnp.exp(ref[...])).astype(BF16), heads).astype(BF16)


def send_all(count, me, make):
    barrier = pltpu.get_barrier_semaphore()
    for step in range(1, count):
        pl.semaphore_signal(
            barrier, inc=1, device_id={"sp": lax.rem(me + step, count)}, device_id_type=MESH
        )
    pl.semaphore_wait(barrier, count - 1)
    copies = []
    for step in range(1, count):
        for copy in make(step, lax.rem(me + step, count), (me + step) // count):
            copy.start()
            copies.append(copy)
    for copy in copies:
        copy.wait()


def chain(count, me, slots, totals, low_cols, high_cols, out_ref):
    shape = out_ref.shape[1:]
    low = jnp.zeros(shape, F32)
    high = jnp.zeros(shape, F32)
    for step in range(count - 1, 0, -1):
        use = (me >= step).astype(F32)
        decay = jnp.exp(totals[step, 0:1, low_cols])
        low = (1.0 - use + use * decay) * low + use * slots[step].astype(F32)
    for step in range(1, count):
        use = (me < step).astype(F32)
        decay = jnp.exp(totals[step, 0:1, high_cols])
        high = (1.0 - use + use * decay) * high + use * slots[step].astype(F32)
    out_ref[0] = low
    out_ref[1] = high


def first_exchange(count, x_ref, tot_ref, out_ref, totals_ref, slots, got, send, recv, tsend, trecv):
    me = lax.axis_index("sp")
    keys = x_ref.shape[2]

    def make(step, target, half):
        return (
            pltpu.make_async_remote_copy(
                src_ref=x_ref.at[half], dst_ref=slots.at[step], send_sem=send.at[step],
                recv_sem=recv.at[step], device_id={"sp": target}, device_id_type=MESH,
            ),
            pltpu.make_async_remote_copy(
                src_ref=tot_ref, dst_ref=got.at[step], send_sem=tsend.at[step],
                recv_sem=trecv.at[step], device_id={"sp": target}, device_id_type=MESH,
            ),
        )

    send_all(count, me, make)
    totals_ref[0] = tot_ref[...]
    for step in range(1, count):
        totals_ref[step] = got[step]
    chain(count, me, slots, got, slice(0, keys), slice(keys, 2 * keys), out_ref)


def second_exchange(count, x_ref, totals_ref, out_ref, slots, send, recv):
    me = lax.axis_index("sp")
    keys = x_ref.shape[2]

    def make(step, target, half):
        return (
            pltpu.make_async_remote_copy(
                src_ref=x_ref.at[half], dst_ref=slots.at[step], send_sem=send.at[step],
                recv_sem=recv.at[step], device_id={"sp": target}, device_id_type=MESH,
            ),
        )

    send_all(count, me, make)
    chain(count, me, slots, totals_ref, slice(keys, 2 * keys), slice(0, keys), out_ref)


def grads_kernel(
    heads, q_ref, k_ref, v_ref, do_ref, cf_ref, cb_ref, st_ref, into_ref, leave_ref,
    dq_ref, dk_ref, dv_ref, df_ref, db_ref,
):
    count, keys = k_ref.shape
    scale = DK**-0.5
    q = q_ref[...].astype(F32) * scale
    k = k_ref[...].astype(F32)
    v = v_ref[...]
    do = do_ref[...]
    lower = triangle(count, True)
    upper = triangle(count, False)
    sides = []
    dv = None
    for side in range(2):
        running = (cf_ref, cb_ref)[side][...]
        total = running[count - 1 : count] if side == 0 else running[0:1]
        up = jnp.exp(running - 0.5 * total)
        down = jnp.exp(0.5 * total - running)
        entering = into_ref[side]
        leaving = leave_ref[1 - side]
        spread_in = jnp.concatenate(
            [jnp.where(head_lanes(h, DK, keys), entering, 0.0) for h in range(heads)], axis=0
        ).astype(BF16)
        spread_out = jnp.concatenate(
            [jnp.where(head_lanes(h, DK, keys), leaving, 0.0) for h in range(heads)], axis=0
        ).astype(BF16)
        tail = jnp.exp(total - running)
        dq = jnp.exp(running) * dot(do, spread_in)
        dk = tail * dot(v, spread_out)
        part = dot((k * tail).astype(BF16), spread_out, ((1,), (1,)))
        dv = part if dv is None else dv + part
        edge = jnp.sum((jnp.exp(total) * entering + st_ref[side]) * leaving, axis=0, keepdims=True)
        sides.append([(q * up).astype(BF16), (k * down).astype(BF16), up, down, dq, dk, edge])
    dv_ref[...] = dv
    inner = [[jnp.zeros((count, keys), F32) for _ in range(2)] for _ in range(2)]
    for head in range(heads):
        pair = slice(head // 2 * 2 * DV, (head // 2 * 2 + 2) * DV)
        half = head_lanes(head % 2, DV, 2 * DV)
        mask = head_lanes(head, DK, keys)
        do_pair = jnp.where(half, do[:, pair], jnp.zeros((), BF16))
        v_pair = v[:, pair]
        weights = dot(do_pair, v_pair, ((1,), (1,)))
        turned = dot(v_pair, do_pair, ((1,), (1,)))
        mixed = None
        for side in range(2):
            q_side, k_side = sides[side][:2]
            q_head = jnp.where(mask, q_side, jnp.zeros((), BF16))
            k_head = jnp.where(mask, k_side, jnp.zeros((), BF16))
            kept, kept_turned = (lower, upper) if side == 0 else (upper, lower)
            scores = jnp.where(kept_turned, dot(k_head, q_side, ((1,), (1,))), 0.0)
            mixed = scores if mixed is None else mixed + scores
            inner[side][0] += dot(jnp.where(kept, weights, 0.0).astype(BF16), k_head)
            inner[side][1] += dot(jnp.where(kept_turned, turned, 0.0).astype(BF16), q_head)
        dv_ref[:, pair] += dot(mixed.astype(BF16), do_pair)
    total_q = None
    for side in range(2):
        up, down, dq, dk, edge = sides[side][2:]
        dq = dq + up * inner[side][0]
        dk = dk + down * inner[side][1]
        gap = q * dq - k * dk
        sums = (upper if side == 0 else lower).astype(F32)
        (df_ref, db_ref)[side][...] = dot(sums, gap, precision=HIGHEST) + edge
        if side == 0:
            total_q, total_k = dq, dk
        else:
            dq_ref[...] = (total_q + dq) * scale
            dk_ref[...] = total_k + dk


def cost(flops, moved):
    return pl.CostEstimate(flops=flops, bytes_accessed=moved, transcendentals=0)


def params(identity=None):
    if identity is None:
        return pltpu.CompilerParams(vmem_limit_bytes=VMEM_LIMIT)
    return pltpu.CompilerParams(
        collective_id=identity, has_side_effects=True, vmem_limit_bytes=VMEM_LIMIT
    )


def shaped(shape, kind=F32):
    return jax.ShapeDtypeStruct(shape, kind)


def mixer_start(key_rows, value_rows, log_forward, log_backward):
    count, keys = key_rows.shape
    heads = keys // DK
    groups = lax.axis_size("sp")
    cf, cb, total, state, state_sent = pl.pallas_call(
        functools.partial(prep_kernel, heads),
        out_shape=(
            shaped((count, keys)), shaped((count, keys)), shaped((8, 2 * keys)),
            shaped((2, DV, keys)), shaped((2, DV, keys), BF16),
        ),
        in_specs=[VMEM] * 4,
        out_specs=(VMEM,) * 5,
        compiler_params=params(),
        cost_estimate=cost(2 * 10**9, 2 * 10**6),
        name="mixer_prep",
    )(key_rows, value_rows, log_forward, log_backward)
    into, totals = pl.pallas_call(
        functools.partial(first_exchange, groups),
        out_shape=(shaped((2, DV, keys)), shaped((groups, 8, 2 * keys))),
        in_specs=[VMEM] * 2,
        out_specs=(VMEM,) * 2,
        scratch_shapes=[
            pltpu.VMEM((groups, DV, keys), BF16), pltpu.VMEM((groups, 8, 2 * keys), F32),
        ] + [pltpu.SemaphoreType.DMA((groups,))] * 4,
        compiler_params=params(1),
        cost_estimate=cost(10**6, 8 * 10**6),
        name="first_exchange",
    )(state_sent, total)
    return cf, cb, state, into, totals


def mixer_grads(query_rows, key_rows, value_rows, mix_grad, started):
    cf, cb, state, into, totals = started
    count, keys = key_rows.shape
    heads = keys // DK
    groups = lax.axis_size("sp")
    pulled = pl.pallas_call(
        functools.partial(pull_kernel, heads),
        out_shape=shaped((2, DV, keys), BF16),
        in_specs=[VMEM] * 4,
        out_specs=VMEM,
        compiler_params=params(),
        cost_estimate=cost(10**9, 10**6),
        name="mixer_pull",
    )(query_rows, mix_grad, cf, cb)
    leave = pl.pallas_call(
        functools.partial(second_exchange, groups),
        out_shape=shaped((2, DV, keys)),
        in_specs=[VMEM] * 2,
        out_specs=VMEM,
        scratch_shapes=[pltpu.VMEM((groups, DV, keys), BF16)]
        + [pltpu.SemaphoreType.DMA((groups,))] * 2,
        compiler_params=params(2),
        cost_estimate=cost(10**6, 8 * 10**6),
        name="second_exchange",
    )(pulled, totals)
    wide = value_rows.shape[1]
    return pl.pallas_call(
        functools.partial(grads_kernel, heads),
        out_shape=tuple(shaped((count, w)) for w in (keys, keys, wide, keys, keys)),
        in_specs=[VMEM] * 9,
        out_specs=(VMEM,) * 5,
        compiler_params=params(),
        cost_estimate=cost(8 * 10**9, 4 * 10**6),
        name="mixer_grads",
    )(query_rows, key_rows, value_rows, mix_grad, cf, cb, state, into, leave)


def dispatch_kernel(
    count, cot_ref, tok_ref, cot_out, tok_out, send, recv, relay_send, relay_recv, own_sem
):
    me = lax.axis_index("sp")
    core = lax.axis_index("tp")
    partner = 1 - core
    width = cot_ref.shape[2]
    columns = pl.ds(pl.multiple_of(core * width, width), width)
    pairs = ((cot_ref, cot_out), (tok_ref, tok_out))
    barrier = pltpu.get_barrier_semaphore()
    for step in range(1, count):
        pl.semaphore_signal(
            barrier, inc=1, device_id={"sp": lax.rem(me + step, count)}, device_id_type=MESH
        )
    pl.semaphore_signal(barrier, inc=1, device_id={"tp": partner}, device_id_type=MESH)
    pl.semaphore_wait(barrier, count)
    sent = []
    for step in range(1, count):
        target = lax.rem(me + step, count)
        for which, (source, result) in enumerate(pairs):
            copy = pltpu.make_async_remote_copy(
                src_ref=source.at[target],
                dst_ref=result.at[me, :, columns],
                send_sem=send.at[which, step],
                recv_sem=recv.at[which, step],
                device_id={"sp": target},
                device_id_type=MESH,
            )
            copy.start()
            sent.append(copy)
    relayed = []
    for which, (source, result) in enumerate(pairs):
        copy = pltpu.make_async_remote_copy(
            src_ref=source.at[me],
            dst_ref=result.at[me, :, columns],
            send_sem=relay_send.at[which, 0],
            recv_sem=relay_recv.at[which, 0],
            device_id={"tp": partner},
            device_id_type=MESH,
        )
        copy.start()
        relayed.append(copy)
    own = [
        pltpu.make_async_copy(source.at[me], result.at[me, :, columns], own_sem.at[which])
        for which, (source, result) in enumerate(pairs)
    ]
    for copy in own:
        copy.start()
    for step in range(1, count):
        origin = lax.rem(me + count - step, count)
        for which, (source, result) in enumerate(pairs):
            landed = result.at[origin, :, columns]
            pltpu.make_async_remote_copy(
                src_ref=source.at[origin],
                dst_ref=landed,
                send_sem=send.at[which, step],
                recv_sem=recv.at[which, step],
                device_id={"sp": origin},
                device_id_type=MESH,
            ).wait_recv()
            copy = pltpu.make_async_remote_copy(
                src_ref=landed,
                dst_ref=landed,
                send_sem=relay_send.at[which, step],
                recv_sem=relay_recv.at[which, step],
                device_id={"tp": partner},
                device_id_type=MESH,
            )
            copy.start()
            relayed.append(copy)
    for copy in sent:
        copy.wait_send()
    for copy in own:
        copy.wait()
    other = pl.ds(pl.multiple_of(partner * width, width), width)
    for copy in relayed:
        copy.wait_send()
    for step in range(count):
        origin = lax.rem(me + count - step, count)
        for which, (source, result) in enumerate(pairs):
            arrived = result.at[origin, :, other]
            pltpu.make_async_remote_copy(
                src_ref=arrived,
                dst_ref=arrived,
                send_sem=relay_send.at[which, step],
                recv_sem=relay_recv.at[which, step],
                device_id={"tp": partner},
                device_id_type=MESH,
            ).wait_recv()


def dispatch(routed_cot, routed_tok):
    groups, slots, width = routed_cot.shape
    whole = shaped((groups, slots, 2 * width), BF16)
    return pl.pallas_call(
        functools.partial(dispatch_kernel, groups),
        out_shape=(whole, whole),
        in_specs=[ANY] * 2,
        out_specs=(ANY,) * 2,
        scratch_shapes=[pltpu.SemaphoreType.DMA((2, groups))] * 4
        + [pltpu.SemaphoreType.DMA((2,))],
        compiler_params=pltpu.CompilerParams(collective_id=3, has_side_effects=True),
        cost_estimate=cost(10**6, 10**8),
        name="dispatch",
    )(routed_cot, routed_tok)


def return_kernel(count, source, result, send, recv, own_sem):
    me = lax.axis_index("sp")
    own = pltpu.make_async_copy(source.at[me], result.at[me], own_sem)
    own.start()

    def make(step, target, half):
        return (
            pltpu.make_async_remote_copy(
                src_ref=source.at[target], dst_ref=result.at[me], send_sem=send.at[step],
                recv_sem=recv.at[step], device_id={"sp": target}, device_id_type=MESH,
            ),
        )

    send_all(count, me, make)
    own.wait()


def send_back(rows):
    groups = rows.shape[0]
    return pl.pallas_call(
        functools.partial(return_kernel, groups),
        out_shape=shaped(rows.shape, BF16),
        in_specs=[ANY],
        out_specs=ANY,
        scratch_shapes=[pltpu.SemaphoreType.DMA((groups,))] * 2 + [pltpu.SemaphoreType.DMA],
        compiler_params=pltpu.CompilerParams(collective_id=4, has_side_effects=True),
        cost_estimate=cost(10**6, 5 * 10**7),
        name="send_back",
    )(rows)


def local(
    cotangent,
    mixed_input,
    route_ids,
    route_gates,
    expert_gate,
    expert_up,
    expert_down,
    projection,
    mixer_output,
    query_rows,
    key_rows,
    value_rows,
    log_forward,
    log_backward,
):
    tok_count = cotangent.shape[0]
    feature_count = cotangent.shape[1]
    groups = lax.axis_size("sp")
    core = lax.axis_index("tp")
    half = feature_count // 2
    slot_count = 4 * tok_count // groups
    row_total = groups * slot_count
    contract_last = ((1,), (1,))
    contract_first = ((0,), (0,))
    swap = [(0, 1), (1, 0)]

    experts = jnp.arange(groups, dtype=jnp.int32)
    chosen = [(route_ids[:, place : place + 1] == experts[None, :]) for place in range(2)]
    named = (chosen[0] | chosen[1]).astype(BF16)
    steps = jnp.arange(tok_count, dtype=jnp.int32)
    before = dot((steps[:, None] > steps[None, :]).astype(BF16), named)
    place_of = before + (experts * slot_count).astype(F32)[None, :]
    rows = jnp.arange(row_total, dtype=jnp.int32)[:, None]
    hits = []
    for place in range(2):
        target = jnp.sum(jnp.where(chosen[place], place_of, 0.0), axis=1).astype(jnp.int32)
        hits.append(rows == target[None, :])
    pick = (hits[0] | hits[1]).astype(BF16)
    slot_gate = jnp.sum(
        jnp.where(hits[0], route_gates[:, 0][None, :], 0.0)
        + jnp.where(hits[1], route_gates[:, 1][None, :], 0.0),
        axis=1,
        keepdims=True,
    )
    own_cot = lax.dynamic_slice_in_dim(cotangent, core * half, half, 1)
    own_tok = lax.dynamic_slice_in_dim(mixed_input, core * half, half, 1)
    routed_cot = (slot_gate * dot(pick, own_cot)).astype(BF16)
    routed_tok = dot(pick, own_tok).astype(BF16)
    started = mixer_start(key_rows, value_rows, log_forward, log_backward)
    routed_cot, routed_tok, started = lax.optimization_barrier((routed_cot, routed_tok, started))
    cot_in, tok_in = dispatch(
        routed_cot.reshape(groups, slot_count, half), routed_tok.reshape(groups, slot_count, half)
    )
    w_gate = expert_gate[0]
    w_up = expert_up[0]
    w_down = expert_down[0]
    cot_block = cot_in.reshape(row_total, feature_count)
    tok_block = tok_in.reshape(row_total, feature_count)
    gate_pre = dot(tok_block, w_gate)
    up_pre = dot(tok_block, w_up)
    sigmoid_gate = jax.nn.sigmoid(gate_pre)
    silu_gate = gate_pre * sigmoid_gate
    hidden = (silu_gate * up_pre).astype(BF16)
    hidden_grad = dot(cot_block, w_down, contract_last)
    slope = sigmoid_gate * (1.0 + gate_pre * (1.0 - sigmoid_gate))
    gate_pre_grad = (hidden_grad * up_pre * slope).astype(BF16)
    up_pre_grad = (hidden_grad * silu_gate).astype(BF16)
    partial_value = dot(gate_pre_grad, w_gate, contract_last)
    partial_value = (partial_value + dot(up_pre_grad, w_up, contract_last)).astype(BF16)
    mine = lax.dynamic_slice_in_dim(partial_value, core * half, half, 1)
    other = lax.dynamic_slice_in_dim(partial_value, (1 - core) * half, half, 1)
    came = lax.ppermute(other, "tp", swap)
    summed = (mine.astype(F32) + came.astype(F32)).astype(BF16)
    returned = send_back(summed.reshape(groups, slot_count, half)).reshape(row_total, half)
    down_term = dot(hidden, cot_block, contract_first)
    gate_term = dot(tok_block, gate_pre_grad, contract_first)
    up_term = dot(tok_block, up_pre_grad, contract_first)
    mid_half = (dot(pick, returned, contract_first) + own_cot.astype(F32)).astype(BF16)
    mid_other = lax.ppermute(mid_half, "tp", swap)
    first = core == 0
    mid_grad = jnp.concatenate(
        [jnp.where(first, mid_half, mid_other), jnp.where(first, mid_other, mid_half)], axis=1
    )
    mix_grad = dot(mid_grad, projection).astype(BF16)
    projection_grad = lax.psum_scatter(
        dot(mid_grad, mixer_output, contract_first), "sp", scatter_dimension=0, tiled=True
    )
    grads = mixer_grads(query_rows, key_rows, value_rows, mix_grad, started)
    return (gate_term[None], up_term[None], down_term[None], projection_grad, *grads)


def solution(mesh):
    rows = P("sp", None)
    both = P("sp", "tp")
    split_last = P("sp", None, "tp")
    split_first = P("sp", "tp", None)
    return jax.shard_map(
        local,
        mesh=mesh,
        in_specs=(
            rows, rows, rows, rows, split_last, split_last, split_first, P(None, "tp"),
            both, both, both, both, both, both,
        ),
        out_specs=(split_last, split_last, split_first, both, both, both, both, both, both),
        check_vma=False,
    )
```
